128 devices in a mesh: sp: 16 (over z, x), tp: 8 (over y, core).
Axes of the slice: x: 4, y: 4, z: 4, core: 2. Of those that a mesh axis runs over, the one named last changes fastest.
Arguments:
- tokens: bfloat16 [8192, 4096], P('sp'), may hold values from -6 to 6
- norm_gain: float32 [4096], replicated, may hold values from 0.1 to 1.9
- w_pool_in: bfloat16 [4096, 2048], P(None, 'tp'), may hold values from -0.09375 to 0.09375
- w_query: bfloat16 [4096, 2048], P(None, 'tp'), may hold values from -0.15625 to 0.15625
- w_key: bfloat16 [4096, 2048], P(None, 'tp'), may hold values from -0.15625 to 0.15625
- w_value: bfloat16 [4096, 2048], P(None, 'tp'), may hold values from -0.09375 to 0.09375
- pool_mix: bfloat16 [32, 64, 64], P('tp'), may hold values from -0.75 to 0.75
- pool_scale: float32 [2048], P('tp'), may hold values from 0.1 to 1.9
- lam: float32 [16], P('tp'), may hold values from 0.3 to 0.8
- head_gain: float32 [128], replicated, may hold values from 0.1 to 1.9
- pool_proj: bfloat16 [2048, 4096], P('tp'), may hold values from -0.125 to 0.125
- attn_proj: bfloat16 [2048, 4096], P('tp'), may hold values from -0.125 to 0.125
Outputs:
- mixed: bfloat16 [8192, 4096], P(('sp', 'tp'))
The draws below stay inside these ranges and needn't reach their ends.
All inputs are finite; a program needn't handle non-finite values.
Results may differ from the reference program's by a relative error of at most 0.015.
Values may be sent and summed in bfloat16 or wider, within the bound.
No kernel may reach another device: no remote copies, remote signals or barrier semaphores. Data moves between devices by JAX's collectives and lax.ppermute only.
A program may use at most 128 MiB of HBM per device.

```python
import jax
import jax.numpy as jnp
from jax import lax

D = 4096
GROUPS = 32
GDIM = 64
HEADS = 16
HEAD = 64
VDIM = 128
SEGMENT = 64
REACH = 16
POOL = 2048
TOKENS = 8192
N_TP = 8


def weight_noise(key, stream_id):
    drawn = 1.3 * jax.random.normal(jax.random.fold_in(key, stream_id), (D, HEADS * 2 * HEAD), jnp.float32)
    return jnp.clip(drawn, -7.8, 7.8) * D ** (-0.5)


def draw_tokens(key, part):
    noise_key = jax.random.fold_in(key, 11)
    drawn = jax.random.normal(noise_key, (TOKENS, D), jnp.float32)
    return jnp.clip(drawn, -6.0, 6.0).astype(jnp.bfloat16)


def draw_w_query(key, part):
    noise_part = weight_noise(key, 21)
    drawn = noise_part
    return drawn.astype(jnp.bfloat16)


def draw_w_key(key, part):
    noise_part = weight_noise(key, 22)
    drawn = noise_part
    return drawn.astype(jnp.bfloat16)


def shard_levels(rng, shape, split, smallest, largest):
    level = 1.0
    for axis_at, shards_of in split:
        heights = jax.random.uniform(jax.random.fold_in(jax.random.fold_in(rng, 6), axis_at), (shards_of,), jnp.float32, smallest / len(split), largest / len(split))
        level = level * jnp.repeat(jnp.exp(heights), shape[axis_at] // shards_of).reshape((-1,) + (1,) * (len(shape) - 1 - axis_at))
    return level


def scatter_about(rng, extent, deviation, most, pieces=(), kind=jnp.bfloat16):
    factor_of = shard_levels(rng, extent, pieces, -0.22, 0.18) if pieces else 1.0
    values = jax.random.normal(rng, extent, jnp.float32) * deviation * factor_of
    return jnp.minimum(jnp.maximum(values, -most), most).astype(kind)


def setup_inputs(seed: int = 0) -> dict:
    splits = jax.random.split(jax.random.key(seed), 13)
    tokens = draw_tokens(jax.random.fold_in(splits[12], 71), 0)
    norm_gain = jnp.clip(1.0 + 0.18 * jax.random.normal(splits[1], (D,), jnp.float32), 0.1, 1.9)
    w_pool_in = scatter_about(splits[2], (D, POOL), D ** -0.5, 0.09375, ((1, 8),))
    w_query = draw_w_query(jax.random.fold_in(splits[12], 71), 0)
    w_key = draw_w_key(jax.random.fold_in(splits[12], 71), 0)
    w_value = scatter_about(splits[5], (D, HEADS * VDIM), D ** -0.5, 0.09375, ((1, 8),))
    pool_mix = scatter_about(splits[6], (GROUPS, GDIM, GDIM), GDIM ** -0.5, 0.75, ((0, 8),))
    pool_scale = jnp.clip(1.0 + 0.18 * jax.random.normal(splits[7], (POOL,), jnp.float32), 0.1, 1.9)
    lam = jnp.clip(0.3 + 0.5 * jax.random.uniform(splits[8], (HEADS,), jnp.float32) ** shard_levels(splits[8], (HEADS,), ((0, 8),), -0.2, 0.2), 0.3, 0.8)
    head_gain = jnp.clip(1.0 + 0.18 * jax.random.normal(splits[9], (VDIM,), jnp.float32), 0.1, 1.9)
    pool_proj = scatter_about(splits[10], (POOL, D), POOL ** -0.5, 0.125, ((0, 8),))
    attn_proj = scatter_about(splits[11], (HEADS * VDIM, D), (HEADS * VDIM) ** -0.5, 0.125, ((0, 8),))
    return {"tokens": tokens, "norm_gain": norm_gain, "w_pool_in": w_pool_in, "w_query": w_query, "w_key": w_key, "w_value": w_value, "pool_mix": pool_mix, "pool_scale": pool_scale, "lam": lam, "head_gain": head_gain, "pool_proj": pool_proj, "attn_proj": attn_proj}


eps_norm = 1e-06
neg_big = -1e+30
out_scale = 0.8

def reference(tokens, norm_gain, w_pool_in, w_query, w_key, w_value, pool_mix, pool_scale, lam, head_gain, pool_proj, attn_proj):
    wide = tokens.astype(jnp.float32)
    normed = (wide * lax.rsqrt(lax.optimization_barrier(jnp.mean(wide * wide, axis=-1, keepdims=True)) + eps_norm) * norm_gain).astype(jnp.bfloat16)
    pool_in = jnp.dot(normed, w_pool_in, preferred_element_type=jnp.float32).astype(jnp.bfloat16)
    query = jnp.dot(normed, w_query, preferred_element_type=jnp.float32).astype(jnp.bfloat16)
    keys = jnp.dot(normed, w_key, preferred_element_type=jnp.float32).astype(jnp.bfloat16)
    values = jnp.dot(normed, w_value, preferred_element_type=jnp.float32).astype(jnp.bfloat16)
    padded = jnp.concatenate([jnp.zeros((REACH - 1, POOL), jnp.float32), pool_in.astype(jnp.float32)], 0)
    channel_group = jnp.arange(POOL, dtype=jnp.int32) // GDIM
    window = 2 ** (1 + channel_group % 4)
    total = jnp.zeros((TOKENS, POOL), jnp.float32)
    for back in range(REACH):
        low = REACH - 1 - back
        total = total + jnp.where(back < window[None, :], padded[low:low + TOKENS], 0.0)
    position = jnp.arange(TOKENS, dtype=jnp.int32)
    count = jnp.minimum(position[:, None] + 1, window[None, :]).astype(jnp.float32)
    pooled = (total / count - pool_in.astype(jnp.float32)).astype(jnp.bfloat16)
    grouped = jnp.einsum('sgi,gio->sgo', pooled.reshape(TOKENS, GROUPS, GDIM).astype(jnp.float32), pool_mix.astype(jnp.float32))
    pool_out = (grouped.reshape(TOKENS, POOL) * pool_scale).astype(jnp.bfloat16)
    query_heads = query.reshape(TOKENS, HEADS, 2, HEAD).transpose(1, 0, 2, 3)
    key_heads = keys.reshape(TOKENS, HEADS, 2, HEAD).transpose(1, 0, 2, 3)
    value_heads = values.reshape(TOKENS, HEADS, VDIM).transpose(1, 0, 2)
    segments = position // SEGMENT
    block = min(TOKENS, 512) if TOKENS % min(TOKENS, 512) == 0 else TOKENS
    scale = HEAD ** (-0.5)

    def one_head(args):
        query_head, key_head, value_head, lam_head = args

        def one_block(index):
            first = (index * block).astype(jnp.int32)
            query_block = lax.dynamic_slice_in_dim(query_head, first, block, 0)
            query_seg = (first + jnp.arange(block, dtype=jnp.int32)) // SEGMENT
            allowed = segments[None, :] <= query_seg[:, None]
            results = []
            for which in range(2):
                scores = jnp.dot(query_block[:, which], key_head[:, which].T, preferred_element_type=jnp.float32) * scale
                masked = jnp.where(allowed, scores, neg_big)
                top = lax.optimization_barrier(jnp.max(masked, axis=-1, keepdims=True))
                probs = jnp.where(allowed, jnp.exp(masked - top), 0.0)
                weighted = jnp.dot(probs.astype(jnp.bfloat16), value_head, preferred_element_type=jnp.float32)
                results.append(weighted / lax.optimization_barrier(jnp.sum(probs, axis=-1, keepdims=True)))
            blend = results[0] - lam_head * results[1]
            scaled = blend * lax.rsqrt(lax.optimization_barrier(jnp.mean(blend * blend, axis=-1, keepdims=True)) + eps_norm) * head_gain * out_scale
            return scaled.astype(jnp.bfloat16)
        return lax.map(one_block, jnp.arange(TOKENS // block, dtype=jnp.int32))
    per_head = lax.map(one_head, (query_heads, key_heads, value_heads, lam))
    attn_out = per_head.reshape(HEADS, TOKENS, VDIM).transpose(1, 0, 2).reshape(TOKENS, HEADS * VDIM)
    pool_share = POOL // N_TP
    attn_share = HEADS * VDIM // N_TP
    summed = jnp.zeros((TOKENS, D), jnp.float32)
    for part in range(N_TP):
        term = jnp.dot(pool_out[:, part * pool_share:(part + 1) * pool_share], pool_proj[part * pool_share:(part + 1) * pool_share], preferred_element_type=jnp.float32)
        term = term + jnp.dot(attn_out[:, part * attn_share:(part + 1) * attn_share], attn_proj[part * attn_share:(part + 1) * attn_share], preferred_element_type=jnp.float32)
        summed = summed + lax.optimization_barrier(term.astype(jnp.bfloat16)).astype(jnp.float32)
    return summed.astype(jnp.bfloat16)
```

```python
import math

import jax
import jax.numpy as jnp
from jax import lax
from jax.experimental import pallas as pl
from jax.experimental.pallas import tpu as pltpu
from jax.sharding import PartitionSpec as P

GDIM = 64
HEAD = 64
VDIM = 128
SEGMENT = 64
REACH = 16
BLK = 512
NB = 16

eps_norm = 1e-06
neg_big = -1e30
out_scale = 0.8

AXES = ("sp", "tp")


def device_of(z, x, y, c):
    return ((z % 4) * 4 + (x % 4)) * 8 + (y % 4) * 2 + (c % 2)


def pairs_of(target):
    pairs = []
    for z in range(4):
        for x in range(4):
            for y in range(4):
                for c in range(2):
                    pairs.append((device_of(z, x, y, c), device_of(*target(z, x, y, c))))
    return pairs


def moved(array, pairs):
    return lax.ppermute(array, AXES, pairs)


def kv_pairs(s, j):
    return pairs_of(lambda z, x, y, c: (z + j, 2 * c + ((x >> 1) ^ s), y, x & 1))


def pair_place(z, x):
    b = z * 4 + x
    p = b if b < 8 else 15 - b
    if p < 4:
        return (3 if p & 1 else 0), p >> 1
    return (2 if p & 1 else 1), (p >> 1) & 1


def q_pairs(s):
    def target(z, x, y, c):
        zeta, kappa = pair_place(z, x)
        e = 1 if z >= 2 else 0
        return zeta, 2 * c + (e ^ s), y, kappa

    return pairs_of(target)


def turned(pairs):
    return [(b, a) for a, b in pairs]


SWAP = pairs_of(lambda z, x, y, c: (z, x, y, c + 1))


def normalize(rows_in, gain):
    wide = rows_in.astype(jnp.float32)
    scaled = wide * lax.rsqrt(jnp.mean(wide * wide, axis=-1, keepdims=True) + eps_norm) * gain
    return scaled.astype(jnp.bfloat16)


def pooling(pool_in, rim, pool_mix, pool_scale, group_first, offset):
    count_rows, width = pool_in.shape
    padded = jnp.concatenate([rim, pool_in], 0).astype(jnp.float32)
    channel_group = group_first + jnp.arange(width, dtype=jnp.int32) // GDIM
    window = 2 ** (1 + channel_group % 4)
    total = jnp.zeros((count_rows, width), jnp.float32)
    for back in range(REACH):
        low = REACH - 1 - back
        total = total + jnp.where(back < window[None, :], padded[low : low + count_rows], 0.0)
    position = offset + jnp.arange(count_rows, dtype=jnp.int32)
    count = jnp.minimum(position[:, None] + 1, window[None, :]).astype(jnp.float32)
    pooled = (total / count - pool_in.astype(jnp.float32)).astype(jnp.bfloat16)
    groups = pool_mix.shape[0]
    grouped = jnp.einsum(
        "sgi,gio->sgo",
        pooled.reshape(count_rows, groups, GDIM),
        pool_mix,
        preferred_element_type=jnp.float32,
    )
    return (grouped.reshape(count_rows, width) * pool_scale).astype(jnp.bfloat16)


def attend_kernel(info, gain_ref, q0_ref, q1_ref, *refs):
    kv_refs = refs[:NB]
    out_refs = refs[NB : NB + 2]
    kvs, acc, top, sems = refs[NB + 2 :]
    copies = []
    for i in range(NB):
        copies.append(pltpu.make_async_copy(kv_refs[i], kvs.at[info[2 + i]], sems.at[i]))
        copies[-1].start()
    for copy in copies:
        copy.wait()
    lane = lax.broadcasted_iota(jnp.int32, (BLK, 128), 1)
    ones = jnp.ones((BLK, 128), jnp.bfloat16)

    for qi, q_ref in enumerate((q0_ref, q1_ref)):
        b_q = info[qi]
        q = q_ref[:BLK]
        maps = (
            jnp.where(lane < HEAD, q, jnp.zeros_like(q)),
            jnp.where(lane < HEAD, jnp.zeros_like(q), q),
        )
        acc[...] = jnp.zeros_like(acc)
        top[...] = jnp.full_like(top, neg_big)

        def block(kb, masked):
            k = kvs[kb, :, :128]
            v = jnp.concatenate([kvs[kb, :, 128:], ones], axis=1)
            for m in range(2):
                s = lax.dot_general(
                    maps[m], k, (((1,), (1,)), ((), ())), preferred_element_type=jnp.float32
                )
                if masked:
                    row = lax.broadcasted_iota(jnp.int32, (BLK, BLK), 0) // SEGMENT
                    col = lax.broadcasted_iota(jnp.int32, (BLK, BLK), 1) // SEGMENT
                    s = jnp.where(col <= row, s, neg_big)
                old = top[m]
                new = jnp.maximum(old, jnp.max(s, axis=1, keepdims=True))
                p = jnp.exp2(s - new[:, :1])
                shrink = jnp.exp2(old - new)
                pv = lax.dot_general(
                    p.astype(jnp.bfloat16),
                    v,
                    (((1,), (0,)), ((), ())),
                    preferred_element_type=jnp.float32,
                )
                acc[m] = acc[m] * jnp.concatenate([shrink, shrink], axis=1) + pv
                top[m] = new

        def step(kb, carry):
            block(kb, False)
            return carry

        lax.fori_loop(0, b_q, step, 0)
        block(b_q, True)
        lam_parts = q_ref[BLK : BLK + 16].astype(jnp.float32)
        lam = (lam_parts[0:1] + lam_parts[1:2]) + lam_parts[2:3]
        blend = acc[0, :, :128] / acc[0, :, 128:] - lam * (acc[1, :, :128] / acc[1, :, 128:])
        scaled = (
            blend
            * lax.rsqrt(jnp.mean(blend * blend, axis=-1, keepdims=True) + eps_norm)
            * gain_ref[...]
            * out_scale
        )
        out_refs[qi][...] = scaled.astype(jnp.bfloat16)


def attend(info, gain, q0, q1, kvs):
    vmem = pl.BlockSpec(memory_space=pltpu.VMEM)
    out = jax.ShapeDtypeStruct((BLK, VDIM), jnp.bfloat16)
    return pl.pallas_call(
        attend_kernel,
        out_shape=(out, out),
        in_specs=[pl.BlockSpec(memory_space=pltpu.SMEM), vmem, vmem, vmem]
        + [pl.BlockSpec(memory_space=pl.ANY)] * NB,
        out_specs=(vmem, vmem),
        scratch_shapes=[
            pltpu.VMEM((NB, BLK, 256), jnp.bfloat16),
            pltpu.VMEM((2, BLK, 256), jnp.float32),
            pltpu.VMEM((2, BLK, 128), jnp.float32),
            pltpu.SemaphoreType.DMA((NB,)),
        ],
        compiler_params=pltpu.CompilerParams(vmem_limit_bytes=40 * 1024 * 1024),
        cost_estimate=pl.CostEstimate(
            flops=17 * 2 * 2 * BLK * BLK * 384, bytes_accessed=NB * BLK * 512, transcendentals=0
        ),
        name="attend",
    )(info, gain, q0, q1, *kvs)


def places():
    sp = lax.axis_index("sp")
    tp = lax.axis_index("tp")
    return sp // 4, sp % 4, tp // 2, tp % 2


def body(
    tokens,
    norm_gain,
    w_pool_in,
    w_query,
    w_key,
    w_value,
    pool_mix,
    pool_scale,
    lam,
    head_gain,
    pool_proj,
    attn_proj,
):
    count_rows = tokens.shape[0]
    z, x, y, c = places()
    b = lax.axis_index("sp")
    offset = b * count_rows
    normed = normalize(tokens, norm_gain)

    def project(weights):
        return jnp.dot(normed, weights, preferred_element_type=jnp.float32)

    keys = project(w_key).astype(jnp.bfloat16)
    values = project(w_value).astype(jnp.bfloat16)
    kv = [
        jnp.concatenate([keys[:, h * 128 : h * 128 + 128], values[:, h * 128 : h * 128 + 128]], 1)
        for h in range(2)
    ]
    flip = (x >> 1) == 1
    kv_s = [jnp.where(flip, kv[1 - s], kv[s]) for s in range(2)]
    own, other, slots_own, slots_other = [], [], [], []
    for j in (0, 1, 3, 2):
        for s in range(2):
            got = moved(kv_s[s], kv_pairs(s, j))
            own.append(got)
            other.append(moved(got, SWAP))
            base = ((z - j) % 4) * 4 + 2 * ((x & 1) ^ s)
            slots_own.append(base + c)
            slots_other.append(base + 1 - c)

    query = (project(w_query) * (HEAD ** (-0.5) * math.log2(math.e))).astype(jnp.bfloat16)
    lam_hi = lam.astype(jnp.bfloat16)
    rest = lam - lax.reduce_precision(lam, 8, 7)
    lam_mid = rest.astype(jnp.bfloat16)
    lam_low = (rest - lax.reduce_precision(rest, 8, 7)).astype(jnp.bfloat16)
    lam_rows = jnp.concatenate(
        [lam_hi[None], lam_mid[None], lam_low[None], jnp.zeros((13, 2), jnp.bfloat16)], 0
    )
    q_heads = [
        jnp.concatenate(
            [
                query[:, h * 128 : h * 128 + 128],
                jnp.broadcast_to(lam_rows[:, h : h + 1], (16, 128)),
            ],
            0,
        )
        for h in range(2)
    ]
    late = z >= 2
    q_s = [jnp.where(late, q_heads[1 - s], q_heads[s]) for s in range(2)]
    got_q = [moved(q_s[s], q_pairs(s)) for s in range(2)]

    middle = (z == 1) | (z == 2)
    odd = (z == 3) | (z == 2)
    place = jnp.where(middle, 4, 0) + 2 * c + jnp.where(odd, 1, 0)
    q_slots = [jnp.where(((x & 1) ^ s) == 0, place, 15 - place) for s in range(2)]
    info = jnp.stack(q_slots + slots_own + slots_other).astype(jnp.int32)

    pool_in = project(w_pool_in).astype(jnp.bfloat16)
    rim = lax.ppermute(pool_in[count_rows - (REACH - 1) :], "sp", [(i, i + 1) for i in range(15)])
    group_first = lax.axis_index("tp") * pool_mix.shape[0]
    pool_out = pooling(pool_in, rim, pool_mix, pool_scale, group_first, offset)

    proj = jnp.concatenate([pool_proj, attn_proj], 0)
    proj_other = moved(proj, SWAP)

    out0, out1 = attend(info, head_gain.reshape(1, VDIM), got_q[0], got_q[1], own + other)
    back = [moved(out, turned(q_pairs(s))) for s, out in enumerate((out0, out1))]
    attn_out = jnp.where(
        late, jnp.concatenate([back[1], back[0]], 1), jnp.concatenate(back, 1)
    )

    acts = jnp.concatenate([pool_out, attn_out], 1).reshape(4, 2, 64, 512)
    mine = jnp.where(c == 0, acts[:, 0], acts[:, 1]).reshape(256, 512)
    theirs = jnp.where(c == 0, acts[:, 1], acts[:, 0]).reshape(256, 512)
    from_partner = moved(theirs, SWAP)
    partial = (
        jnp.dot(mine, proj, preferred_element_type=jnp.float32)
        + jnp.dot(from_partner, proj_other, preferred_element_type=jnp.float32)
    ).astype(jnp.bfloat16)
    blocks = partial.reshape(4, 64, 4096)
    total = lax.dynamic_index_in_dim(blocks, y, 0, keepdims=False).astype(jnp.float32)
    for k in (2, 1, 3):
        piece = lax.dynamic_index_in_dim(blocks, (y + k) % 4, 0, keepdims=False)
        got = moved(piece, pairs_of(lambda z, x, y, c: (z, x, y + k, c)))
        total = total + got.astype(jnp.float32)
    return total.astype(jnp.bfloat16)


def solution(mesh):
    return jax.shard_map(
        body,
        mesh=mesh,
        in_specs=(
            P("sp", None),
            P(),
            P(None, "tp"),
            P(None, "tp"),
            P(None, "tp"),
            P(None, "tp"),
            P("tp", None, None),
            P("tp"),
            P("tp"),
            P(),
            P("tp", None),
            P("tp", None),
        ),
        out_specs=P(("sp", "tp"), None),
        check_vma=False,
    )
```

```python
import math

import jax
import jax.numpy as jnp
from jax import lax
from jax.experimental import pallas as pl
from jax.experimental.pallas import tpu as pltpu
from jax.sharding import PartitionSpec as P


GDIM = 64
HEAD = 64
VDIM = 128
SEGMENT = 64
BLK = 512
NB = 16

eps_norm = 1e-06
neg_big = -1e30
out_scale = 0.8

AXES = ("sp", "tp")


def device_of(z, x, y, c):
    return ((z % 4) * 4 + (x % 4)) * 8 + (y % 4) * 2 + (c % 2)


def pairs_of(target):
    pairs = []
    for z in range(4):
        for x in range(4):
            for y in range(4):
                for c in range(2):
                    pairs.append((device_of(z, x, y, c), device_of(*target(z, x, y, c))))
    return pairs


def moved(array, pairs):
    return lax.ppermute(array, AXES, pairs)


def kv_pairs(s):
    return pairs_of(lambda z, x, y, c: (z, 2 * c + ((x >> 1) ^ s), y, x & 1))


def pair_place(z, x):
    b = z * 4 + x
    p = b if b < 8 else 15 - b
    if p < 4:
        return (3 if p & 1 else 0), p >> 1
    return (2 if p & 1 else 1), (p >> 1) & 1


def q_pairs(s):
    def target(z, x, y, c):
        zeta, kappa = pair_place(z, x)
        e = 1 if z >= 2 else 0
        return zeta, 2 * c + (e ^ s), y, kappa

    return pairs_of(target)


def back_pairs(s, t):
    pairs = []
    for z in range(4):
        for x in range(4):
            zeta, kappa = pair_place(z, x)
            e = 1 if z >= 2 else 0
            for y in range(4):
                for high in range(2):
                    source = device_of(zeta, 2 * high + (e ^ s), y, kappa)
                    pairs.append((source, device_of(z, x, y, high ^ t)))
    return pairs


SWAP = pairs_of(lambda z, x, y, c: (z, x, y, c + 1))
UP = pairs_of(lambda z, x, y, c: (z + 1, x, y, c))
DOWN = pairs_of(lambda z, x, y, c: (z - 1, x, y, c))


F32 = jnp.float32
BF16 = jnp.bfloat16
SMEM_SPEC = pl.BlockSpec(memory_space=pltpu.SMEM)
VMEM_SPEC = pl.BlockSpec(memory_space=pltpu.VMEM)
ANY_SPEC = pl.BlockSpec(memory_space=pl.ANY)


def dot(a, b):
    return jnp.dot(a, b, preferred_element_type=F32)


STEPS = 4


def kv_kernel(place, tok_ref, gain_ref, wk_ref, wv_ref, kv0_ref, kv1_ref, inv_ref, acc, squares):
    i = pl.program_id(0)
    wide = tok_ref[...].astype(F32)
    weighed = (wide * gain_ref[...]).astype(BF16)
    both = jnp.concatenate([wk_ref[...], wv_ref[...]], 1)
    part = dot(weighed, both)
    square = wide * wide
    folded = square[:, :128]
    for k in range(1, wide.shape[1] // 128):
        folded = folded + square[:, k * 128 : (k + 1) * 128]

    @pl.when(i == 0)
    def _():
        acc[...] = part
        squares[...] = folded

    @pl.when(i > 0)
    def _():
        acc[...] += part
        squares[...] += folded

    @pl.when(i == STEPS - 1)
    def _():
        width = wide.shape[1] * STEPS
        inv = lax.rsqrt(jnp.sum(squares[...], axis=-1, keepdims=True) / width + eps_norm)
        inv_ref[...] = jnp.broadcast_to(inv, inv_ref.shape)
        flip = place[1] >= 2
        heads = []
        for h in range(2):
            keys = (acc[:, h * 128 : h * 128 + 128] * inv).astype(BF16)
            values = (acc[:, 256 + h * 128 : 384 + h * 128] * inv).astype(BF16)
            heads.append(jnp.concatenate([keys, values], 1))

        @pl.when(flip)
        def _():
            kv0_ref[...] = heads[1]
            kv1_ref[...] = heads[0]

        @pl.when(jnp.logical_not(flip))
        def _():
            kv0_ref[...] = heads[0]
            kv1_ref[...] = heads[1]


def make_kv(place, tokens, gain, w_key, w_value):
    rows, width = tokens.shape
    chunk = width // STEPS
    weight = pl.BlockSpec((chunk, 256), lambda i: (i, 0))
    kv = jax.ShapeDtypeStruct((rows, 256), BF16)
    whole = pl.BlockSpec((rows, 256), lambda i: (0, 0))
    return pl.pallas_call(
        kv_kernel,
        grid=(STEPS,),
        out_shape=(kv, kv, jax.ShapeDtypeStruct((rows, 128), F32)),
        in_specs=[
            SMEM_SPEC,
            pl.BlockSpec((rows, chunk), lambda i: (0, i)),
            pl.BlockSpec((1, chunk), lambda i: (0, i)),
            weight,
            weight,
        ],
        out_specs=(whole, whole, pl.BlockSpec((rows, 128), lambda i: (0, 0))),
        scratch_shapes=[pltpu.VMEM((rows, 512), F32), pltpu.VMEM((rows, 128), F32)],
        compiler_params=pltpu.CompilerParams(vmem_limit_bytes=60 * 1024 * 1024),
        cost_estimate=pl.CostEstimate(
            flops=2 * rows * width * 512, bytes_accessed=rows * width * 2, transcendentals=0
        ),
        name="make_kv",
    )(place, tokens, gain, w_key, w_value)


def q_kernel(
    place, lam, tok_ref, gain_ref, inv_ref, wq_ref, wp_ref, q0_ref, q1_ref, pool_ref, rim_ref, acc
):
    i = pl.program_id(0)
    weighed = (tok_ref[...].astype(F32) * gain_ref[...]).astype(BF16)
    part = dot(weighed, jnp.concatenate([wq_ref[...], wp_ref[...]], 1))

    @pl.when(i == 0)
    def _():
        acc[...] = part

    @pl.when(i > 0)
    def _():
        acc[...] += part

    def lam_rows(value):
        spread = jnp.full((16, 128), value, F32)
        high = spread.astype(BF16).astype(F32)
        middle = (spread - high).astype(BF16).astype(F32)
        low = spread - high - middle
        row = lax.broadcasted_iota(jnp.int32, (16, 128), 0)
        picked = jnp.where(row == 0, high, jnp.where(row == 1, middle, jnp.where(row == 2, low, 0.0)))
        return picked.astype(BF16)

    @pl.when(i == STEPS - 1)
    def _():
        inv = inv_ref[...]
        factor = inv * (HEAD ** (-0.5) * math.log2(math.e))
        first = (acc[:, :128] * factor).astype(BF16)
        second = (acc[:, 128:256] * factor).astype(BF16)
        late = place[0] >= 2

        @pl.when(late)
        def _():
            q0_ref[:BLK, :] = second
            q1_ref[:BLK, :] = first
            q0_ref[BLK:, :] = lam_rows(lam[1])
            q1_ref[BLK:, :] = lam_rows(lam[0])

        @pl.when(jnp.logical_not(late))
        def _():
            q0_ref[:BLK, :] = first
            q1_ref[:BLK, :] = second
            q0_ref[BLK:, :] = lam_rows(lam[0])
            q1_ref[BLK:, :] = lam_rows(lam[1])

        pool_in = (acc[:, 256:] * jnp.concatenate([inv, inv], 1)).astype(BF16)
        pool_ref[...] = pool_in
        rim_ref[...] = pool_in[BLK - 16 :]


def make_q(place, lam, tokens, gain, inv, w_query, w_pool_in):
    rows, width = tokens.shape
    chunk = width // STEPS
    weight = pl.BlockSpec((chunk, 256), lambda i: (i, 0))
    payload = pl.BlockSpec((rows + 16, 128), lambda i: (0, 0))
    q = jax.ShapeDtypeStruct((rows + 16, 128), BF16)
    return pl.pallas_call(
        q_kernel,
        grid=(STEPS,),
        out_shape=(
            q,
            q,
            jax.ShapeDtypeStruct((rows, 256), BF16),
            jax.ShapeDtypeStruct((16, 256), BF16),
        ),
        in_specs=[
            SMEM_SPEC,
            SMEM_SPEC,
            pl.BlockSpec((rows, chunk), lambda i: (0, i)),
            pl.BlockSpec((1, chunk), lambda i: (0, i)),
            pl.BlockSpec((rows, 128), lambda i: (0, 0)),
            weight,
            weight,
        ],
        out_specs=(
            payload,
            payload,
            pl.BlockSpec((rows, 256), lambda i: (0, 0)),
            pl.BlockSpec((16, 256), lambda i: (0, 0)),
        ),
        scratch_shapes=[pltpu.VMEM((rows, 512), F32)],
        compiler_params=pltpu.CompilerParams(vmem_limit_bytes=60 * 1024 * 1024),
        cost_estimate=pl.CostEstimate(
            flops=2 * rows * width * 512, bytes_accessed=rows * width * 2, transcendentals=0
        ),
        name="make_q",
    )(place, lam, tokens, gain, inv, w_query, w_pool_in)


def pool_kernel(place, pool_ref, rim_ref, mix_ref, scale_ref, mine_ref, theirs_ref, spread, result):
    core = place[3]
    rows, width = pool_ref.shape
    pool_in = pool_ref[...].astype(F32)
    total = jnp.concatenate([rim_ref[...].astype(F32), pool_in], 0)
    group = lax.broadcasted_iota(jnp.int32, (rows + 16, width), 1) // GDIM
    chosen = total
    for level in range(4):
        total = total + pltpu.roll(total, 2**level, 0)
        chosen = total if level == 0 else jnp.where(group >= level, total, chosen)
    position = place[4] + lax.broadcasted_iota(jnp.int32, (rows, width), 0)
    lane_group = lax.broadcasted_iota(jnp.int32, (rows, width), 1) // GDIM
    window = jnp.left_shift(2, lane_group)
    count = jnp.minimum(position + 1, window).astype(F32)
    pooled = (chosen[16:] / count - pool_in).astype(BF16)
    spread[...] = jnp.zeros_like(spread)
    for g in range(width // GDIM):
        spread[g * GDIM : (g + 1) * GDIM, g * GDIM : (g + 1) * GDIM] = mix_ref[g]
    result[...] = dot(pooled, spread[...]) * scale_ref[...]
    for k in range(4):
        here = pl.ds(pl.multiple_of((2 * k + core) * 64, 64), 64)
        there = pl.ds(pl.multiple_of((2 * k + 1 - core) * 64, 64), 64)
        mine_ref[k * 64 : (k + 1) * 64, :] = result[here, :].astype(BF16)
        theirs_ref[k * 64 : (k + 1) * 64, :] = result[there, :].astype(BF16)


def make_pool(place, pool_in, rim, pool_mix, pool_scale):
    rows, width = pool_in.shape
    half = jax.ShapeDtypeStruct((rows // 2, width), BF16)
    return pl.pallas_call(
        pool_kernel,
        out_shape=(half, half),
        in_specs=[SMEM_SPEC] + [VMEM_SPEC] * 4,
        out_specs=(VMEM_SPEC, VMEM_SPEC),
        scratch_shapes=[pltpu.VMEM((width, width), BF16), pltpu.VMEM((rows, width), F32)],
        compiler_params=pltpu.CompilerParams(vmem_limit_bytes=24 * 1024 * 1024),
        cost_estimate=pl.CostEstimate(
            flops=2 * 1024 * 1024 * 1024, bytes_accessed=rows * width * 4, transcendentals=0
        ),
        name="make_pool",
    )(place, pool_in, rim, pool_mix, pool_scale)


def attend_kernel(info, gain_ref, q0_ref, q1_ref, *refs):
    kv_refs = refs[:NB]
    out_refs = refs[NB : NB + 4]
    kvs, acc, top, kept, sems = refs[NB + 4 :]
    copies = []
    for i in range(NB):
        copies.append(pltpu.make_async_copy(kv_refs[i], kvs.at[info[3 + i]], sems.at[i]))
        copies[-1].start()
    for copy in copies:
        copy.wait()
    high = info[2]
    lane = lax.broadcasted_iota(jnp.int32, (BLK, 128), 1)
    low_half = lane < HEAD
    ones = jnp.ones((BLK, 128), BF16)
    zeros = jnp.zeros((BLK, 128), BF16)

    def scores(q, k):
        return lax.dot_general(q, k, (((1,), (1,)), ((), ())), preferred_element_type=F32)

    def diagonal_mask(s):
        row = lax.broadcasted_iota(jnp.int32, (BLK, BLK), 0) // SEGMENT
        col = lax.broadcasted_iota(jnp.int32, (BLK, BLK), 1) // SEGMENT
        return jnp.where(col <= row, s, neg_big)

    for qi, q_ref in enumerate((q0_ref, q1_ref)):
        b_q = info[qi]
        q = q_ref[:BLK]
        maps = (jnp.where(low_half, q, zeros), jnp.where(low_half, zeros, q))

        k = kvs[b_q, :, :128]
        v = jnp.concatenate([kvs[b_q, :, 128:], ones], axis=1)
        shifted = []
        for m in range(2):
            s = diagonal_mask(scores(maps[m], k))
            peak = jnp.max(s, axis=1, keepdims=True).astype(BF16)
            p = jnp.exp2(s - peak.astype(F32))
            acc[m] = dot(p.astype(BF16), v)
            spot = lane == (HEAD if m == 0 else 0)
            shifted.append(jnp.where(spot, -peak, maps[m]))

        def step(kb, carry):
            k = kvs[kb, :, :128]
            v = jnp.concatenate([kvs[kb, :, 128:], ones], axis=1)
            for m in range(2):
                k_one = jnp.where(low_half, k, ones) if m == 0 else jnp.where(low_half, ones, k)
                p = jnp.exp2(scores(shifted[m], k_one))
                acc[m] += dot(p.astype(BF16), v)
            return carry

        lax.fori_loop(0, b_q, step, 0)
        largest = jnp.max(acc[:, :, 128:])

        @pl.when(jnp.logical_not(largest < 2.0**100))
        def _():
            acc[...] = jnp.zeros_like(acc)
            top[...] = jnp.full_like(top, neg_big)

            def careful(kb, carry):
                k = kvs[kb, :, :128]
                v = jnp.concatenate([kvs[kb, :, 128:], ones], axis=1)
                for m in range(2):
                    s = scores(maps[m], k)
                    s = jnp.where(kb == b_q, diagonal_mask(s), s)
                    old = top[m]
                    new = jnp.maximum(old, jnp.max(s, axis=1, keepdims=True))
                    p = jnp.exp2(s - new[:, :1])
                    shrink = jnp.exp2(old - new)
                    acc[m] = acc[m] * jnp.concatenate([shrink, shrink], axis=1) + dot(
                        p.astype(BF16), v
                    )
                    top[m] = new
                return carry

            lax.fori_loop(0, b_q + 1, careful, 0)

        lam_parts = q_ref[BLK : BLK + 16].astype(F32)
        lam = (lam_parts[0:1] + lam_parts[1:2]) + lam_parts[2:3]
        blend = acc[0, :, :128] / acc[0, :, 128:] - lam * (acc[1, :, :128] / acc[1, :, 128:])
        kept[...] = (
            blend
            * lax.rsqrt(jnp.mean(blend * blend, axis=-1, keepdims=True) + eps_norm)
            * gain_ref[...]
            * out_scale
        )
        for t in range(2):
            side = high if t == 0 else 1 - high
            for n in range(4):
                rows = pl.ds(pl.multiple_of((2 * n + side) * 64, 64), 64)
                out_refs[2 * qi + t][n * 64 : (n + 1) * 64, :] = kept[rows, :].astype(BF16)


def attend(info, gain, q0, q1, kvs):
    out = jax.ShapeDtypeStruct((BLK // 2, VDIM), BF16)
    return pl.pallas_call(
        attend_kernel,
        out_shape=(out,) * 4,
        in_specs=[SMEM_SPEC, VMEM_SPEC, VMEM_SPEC, VMEM_SPEC] + [ANY_SPEC] * NB,
        out_specs=(VMEM_SPEC,) * 4,
        scratch_shapes=[
            pltpu.VMEM((NB, BLK, 256), BF16),
            pltpu.VMEM((2, BLK, 256), F32),
            pltpu.VMEM((2, BLK, 128), F32),
            pltpu.VMEM((BLK, 128), F32),
            pltpu.SemaphoreType.DMA((NB,)),
        ],
        compiler_params=pltpu.CompilerParams(vmem_limit_bytes=40 * 1024 * 1024),
        cost_estimate=pl.CostEstimate(
            flops=17 * 2 * 2 * BLK * BLK * 384, bytes_accessed=NB * BLK * 512, transcendentals=0
        ),
        name="attend",
    )(info, gain, q0, q1, *kvs)


COLS = 1024


def proj_kernel(place, pm, po, a00, a01, a10, a11, wp, wa, wpo, wao, own_ref, f1, f2, f3, part):
    y = place[2]
    e = place[5]
    total = dot(pm[...], wp[...]) + dot(po[...], wpo[...])
    for a, b, w in ((a00, a10, wa), (a01, a11, wao)):
        first = jnp.where(e == 0, a[...], b[...])
        second = jnp.where(e == 0, b[...], a[...])
        total += dot(jnp.concatenate([first, second], 1), w[...])
    part[...] = total
    for k, ref in enumerate((own_ref, f1, f2, f3)):
        block = lax.rem(y + k, 4)
        rows = pl.ds(pl.multiple_of(block * 64, 64), 64)
        ref[...] = part[rows, :].astype(ref.dtype)


def project_out(place, pools, backs, weights):
    out_cols = weights[0].shape[1]
    act = pl.BlockSpec((256, 256), lambda i: (0, 0))
    head = pl.BlockSpec((256, 128), lambda i: (0, 0))
    weight = pl.BlockSpec((256, COLS), lambda i: (0, i))
    tile = pl.BlockSpec((64, COLS), lambda i: (0, i))
    piece = jax.ShapeDtypeStruct((64, out_cols), BF16)
    return pl.pallas_call(
        proj_kernel,
        grid=(out_cols // COLS,),
        out_shape=(jax.ShapeDtypeStruct((64, out_cols), F32), piece, piece, piece),
        in_specs=[SMEM_SPEC, act, act] + [head] * 4 + [weight] * 4,
        out_specs=(tile,) * 4,
        scratch_shapes=[pltpu.VMEM((256, COLS), F32)],
        compiler_params=pltpu.CompilerParams(vmem_limit_bytes=32 * 1024 * 1024),
        cost_estimate=pl.CostEstimate(
            flops=2 * 256 * 1024 * out_cols, bytes_accessed=8 * 1024 * 1024, transcendentals=0
        ),
        name="project_out",
    )(place, *pools, *backs, *weights)


def body(
    tokens,
    norm_gain,
    w_pool_in,
    w_query,
    w_key,
    w_value,
    pool_mix,
    pool_scale,
    lam,
    head_gain,
    pool_proj,
    attn_proj,
):
    rows, width = tokens.shape
    sp = lax.axis_index("sp")
    tp = lax.axis_index("tp")
    z, x, y, c = sp // 4, sp % 4, tp // 2, tp % 2
    e = z // 2
    place = jnp.stack([z, x, y, c, sp * rows, e]).astype(jnp.int32)
    gain = norm_gain.reshape(1, width)

    kv0, kv1, inv = make_kv(place, tokens, gain, w_key, w_value)
    own, slots = [], []

    def keep(array, steps, s):
        own.append(array)
        slots.append(((z + steps) % 4) * 4 + 2 * ((x & 1) ^ s))

    g0, g1 = moved(kv0, kv_pairs(0)), moved(kv1, kv_pairs(1))
    q0, q1, pool_in, rim = make_q(place, lam, tokens, gain, inv, w_query, w_pool_in)
    g0, g1, q0, q1, pool_in, rim = lax.optimization_barrier((g0, g1, q0, q1, pool_in, rim))
    up0, down1 = moved(g0, UP), moved(g1, DOWN)
    down0, up1 = moved(g0, DOWN), moved(g1, UP)
    far0, far1 = moved(up0, UP), moved(down1, DOWN)
    keep(g0, 0, 0)
    keep(g1, 0, 1)
    keep(up0, 3, 0)
    keep(down1, 1, 1)
    keep(down0, 1, 0)
    keep(up1, 3, 1)
    keep(far0, 2, 0)
    keep(far1, 2, 1)
    other = [moved(array, SWAP) for array in own]

    got_q = [moved(q0, q_pairs(0)), moved(q1, q_pairs(1))]
    rim = lax.ppermute(rim, "sp", [(i, i + 1) for i in range(15)])
    pool_mine, pool_theirs = make_pool(place, pool_in, rim, pool_mix, pool_scale.reshape(1, -1))
    pool_other = moved(pool_theirs, SWAP)
    pool_proj_other = moved(pool_proj, SWAP)
    attn_proj_other = moved(attn_proj, SWAP)

    middle = (z == 1) | (z == 2)
    odd = (z == 3) | (z == 2)
    spot = jnp.where(middle, 4, 0) + 2 * c + jnp.where(odd, 1, 0)
    q_slots = [jnp.where(((x & 1) ^ s) == 0, spot, 15 - spot) for s in range(2)]
    info = jnp.stack(
        q_slots + [x >> 1] + [i + c for i in slots] + [i + 1 - c for i in slots]
    ).astype(jnp.int32)

    outs = attend(info, head_gain.reshape(1, VDIM), got_q[0], got_q[1], own + other)
    backs = [moved(outs[2 * s + t], back_pairs(s, t)) for s in range(2) for t in range(2)]
    mine, *pieces = project_out(
        place,
        (pool_mine, pool_other),
        backs,
        (pool_proj, attn_proj, pool_proj_other, attn_proj_other),
    )
    total = mine
    for k, piece in zip((1, 2, 3), pieces):
        total = total + moved(piece, pairs_of(lambda z, x, y, c: (z, x, y + k, c))).astype(F32)
    return total.astype(BF16)


def solution(mesh):
    return jax.shard_map(
        body,
        mesh=mesh,
        in_specs=(
            P("sp", None),
            P(),
            P(None, "tp"),
            P(None, "tp"),
            P(None, "tp"),
            P(None, "tp"),
            P("tp", None, None),
            P("tp"),
            P("tp"),
            P(),
            P("tp", None),
            P("tp", None),
        ),
        out_specs=P(("sp", "tp"), None),
        check_vma=False,
    )
```

```python
import functools
import math

import jax
import jax.numpy as jnp
from jax import lax
from jax.experimental import pallas as pl
from jax.experimental.pallas import tpu as pltpu
from jax.sharding import PartitionSpec as P


GDIM = 64
HEAD = 64
VDIM = 128
SEGMENT = 64
BLK = 512
NB = 16
HALF = 8
SAMPLE = 128

eps_norm = 1e-06
neg_big = -1e30
out_scale = 0.8

AXES = ("sp", "tp")


def device_of(z, x, y, c):
    return ((z % 4) * 4 + (x % 4)) * 8 + (y % 4) * 2 + (c % 2)


def pairs_of(target):
    pairs = []
    for z in range(4):
        for x in range(4):
            for y in range(4):
                for c in range(2):
                    pairs.append((device_of(z, x, y, c), device_of(*target(z, x, y, c))))
    return pairs


def moved(array, pairs):
    return lax.ppermute(array, AXES, pairs)


def kv_pairs(s):
    return pairs_of(
        lambda z, x, y, c: (z, 2 * c + ((x & 1) ^ (x >> 1) ^ c ^ s), y, x & 1)
    )


def pair_place(z, x):
    b = z * 4 + x
    p = b if b < 8 else 15 - b
    if p < 4:
        return (3 if p & 1 else 0), p >> 1
    return (2 if p & 1 else 1), (p >> 1) & 1


def q_pairs(s):
    def target(z, x, y, c):
        zeta, kappa = pair_place(z, x)
        e = 1 if z >= 2 else 0
        return zeta, 2 * c + (e ^ s), y, kappa

    return pairs_of(target)


def back_pairs(s):
    return [(b, a) for a, b in q_pairs(s)]


SWAP = pairs_of(lambda z, x, y, c: (z, x, y, c + 1))
UP = pairs_of(lambda z, x, y, c: (z + 1, x, y, c))
DOWN = pairs_of(lambda z, x, y, c: (z - 1, x, y, c))
Y_UP = pairs_of(lambda z, x, y, c: (z, x, y + 1, c))
Y_DOWN = pairs_of(lambda z, x, y, c: (z, x, y - 1, c))


F32 = jnp.float32
BF16 = jnp.bfloat16
SMEM_SPEC = pl.BlockSpec(memory_space=pltpu.SMEM)
VMEM_SPEC = pl.BlockSpec(memory_space=pltpu.VMEM)


def dot(a, b):
    return jnp.dot(a, b, preferred_element_type=F32)


STEPS = 4


def coords():
    sp, tp = lax.axis_index("sp"), lax.axis_index("tp")
    return lax.div(sp, 4), lax.rem(sp, 4), lax.div(tp, 2), lax.rem(tp, 2)


def front_kernel(
    lam, gain_ref, tok, wk, wv, wq, wp, kv0, kv1, q0, q1, pool, rim, toks, weights, acc, squares, sems
):
    rows, width = tok.shape
    chunk = width // STEPS

    def copies(i):
        here = pl.ds(pl.multiple_of(i * chunk, chunk), chunk)
        found = [pltpu.make_async_copy(tok.at[:, here], toks.at[i], sems.at[i, 0])]
        for k, w in enumerate((wk, wv, wq, wp)):
            there = weights.at[i, :, k * 256 : (k + 1) * 256]
            found.append(pltpu.make_async_copy(w.at[here, :], there, sems.at[i, 1 + k]))
        return found

    for i in range(2):
        for copy in copies(i):
            copy.start()
    acc[...] = jnp.zeros_like(acc)
    squares[...] = jnp.zeros_like(squares)

    def step(i, carry):
        for copy in copies(i):
            copy.wait()

        @pl.when(i + 2 < STEPS)
        def _():
            for copy in copies(i + 2):
                copy.start()

        for r in range(2):
            part = slice(r * (rows // 2), (r + 1) * (rows // 2))
            wide = toks[i, part, :].astype(F32)
            weighed = (wide * gain_ref[i]).astype(BF16)
            square = wide * wide
            folded = square[:, :128]
            for k in range(1, chunk // 128):
                folded = folded + square[:, k * 128 : (k + 1) * 128]
            acc[part, :] += dot(weighed, weights[i])
            squares[part, :] += folded
        return carry

    lax.fori_loop(0, STEPS, step, 0)
    z, x, _, c = coords()
    inv = lax.rsqrt(jnp.sum(squares[...], axis=-1, keepdims=True) / width + eps_norm)
    factor = inv * (HEAD ** (-0.5) * math.log2(math.e))
    flip = lax.rem(x + lax.div(x, 2) + c, 2) == 1
    for h in range(2):
        keys = (acc[:, h * 128 : h * 128 + 128] * inv).astype(BF16)
        values = (acc[:, 256 + h * 128 : 384 + h * 128] * inv).astype(BF16)
        query = (acc[:, 512 + h * 128 : 640 + h * 128] * factor).astype(BF16)

        def put_kv(kv):
            kv[:, :128] = keys
            kv[:, 128:] = values

        def put_q(q):
            q[:BLK, :] = query
            q[BLK:, :] = lam_rows(lam[h])

        pl.when(flip)(functools.partial(put_kv, (kv1, kv0)[h]))
        pl.when(jnp.logical_not(flip))(functools.partial(put_kv, (kv0, kv1)[h]))
        pl.when(z >= 2)(functools.partial(put_q, (q1, q0)[h]))
        pl.when(z < 2)(functools.partial(put_q, (q0, q1)[h]))
    pool_in = (acc[:, 768:] * inv).astype(BF16)
    pool[...] = pool_in
    rim[...] = pool_in[rows - 16 :]


def lam_rows(value):
    spread = jnp.full((16, 128), value, F32)
    high = spread.astype(BF16).astype(F32)
    middle = (spread - high).astype(BF16).astype(F32)
    low = spread - high - middle
    row = lax.broadcasted_iota(jnp.int32, (16, 128), 0)
    picked = jnp.where(row == 0, high, jnp.where(row == 1, middle, jnp.where(row == 2, low, 0.0)))
    return picked.astype(BF16)


def make_front(lam, gain, tokens, *weights):
    rows, width = tokens.shape
    chunk = width // STEPS
    kv = jax.ShapeDtypeStruct((rows, 256), BF16)
    q = jax.ShapeDtypeStruct((rows + 16, 128), BF16)
    return pl.pallas_call(
        front_kernel,
        out_shape=(kv, kv, q, q, kv, jax.ShapeDtypeStruct((16, 256), BF16)),
        in_specs=[SMEM_SPEC, VMEM_SPEC] + [pl.BlockSpec(memory_space=pltpu.HBM)] * 5,
        out_specs=(VMEM_SPEC,) * 6,
        scratch_shapes=[
            pltpu.VMEM((STEPS, rows, chunk), BF16),
            pltpu.VMEM((STEPS, chunk, 1024), BF16),
            pltpu.VMEM((rows, 1024), F32),
            pltpu.VMEM((rows, 128), F32),
            pltpu.SemaphoreType.DMA((STEPS, 5)),
        ],
        compiler_params=pltpu.CompilerParams(vmem_limit_bytes=63 * 1024 * 1024),
        cost_estimate=pl.CostEstimate(
            flops=2 * rows * width * 1024, bytes_accessed=rows * width * 6, transcendentals=0
        ),
        name="make_front",
    )(lam, gain, tokens, *weights)


def pool_kernel(pool_ref, rim_ref, mix_ref, scale_ref, mine_ref, theirs_ref, spread, result):
    z, x, _, core = coords()
    rows, width = pool_ref.shape
    pool_in = pool_ref[...].astype(F32)
    total = jnp.concatenate([rim_ref[...].astype(F32), pool_in], 0)
    group = lax.broadcasted_iota(jnp.int32, (rows + 16, width), 1) // GDIM
    chosen = total
    for level in range(4):
        total = total + pltpu.roll(total, 2**level, 0)
        chosen = total if level == 0 else jnp.where(group >= level, total, chosen)
    position = (z * 4 + x) * rows + lax.broadcasted_iota(jnp.int32, (rows, width), 0)
    lane_group = lax.broadcasted_iota(jnp.int32, (rows, width), 1) // GDIM
    window = jnp.left_shift(2, lane_group)
    count = jnp.minimum(position + 1, window).astype(F32)
    pooled = (chosen[16:] / count - pool_in).astype(BF16)
    spread[...] = jnp.zeros_like(spread)
    for g in range(width // GDIM):
        spread[g * GDIM : (g + 1) * GDIM, g * GDIM : (g + 1) * GDIM] = mix_ref[g]
    result[...] = dot(pooled, spread[...]) * scale_ref[...]
    for k in range(4):
        here = pl.ds(pl.multiple_of((2 * k + core) * 64, 64), 64)
        there = pl.ds(pl.multiple_of((2 * k + 1 - core) * 64, 64), 64)
        mine_ref[k * 64 : (k + 1) * 64, :] = result[here, :].astype(BF16)
        theirs_ref[k * 64 : (k + 1) * 64, :] = result[there, :].astype(BF16)


def make_pool(pool_in, rim, pool_mix, pool_scale):
    rows, width = pool_in.shape
    half = jax.ShapeDtypeStruct((rows // 2, width), BF16)
    return pl.pallas_call(
        pool_kernel,
        out_shape=(half, half),
        in_specs=[VMEM_SPEC] * 4,
        out_specs=(VMEM_SPEC, VMEM_SPEC),
        scratch_shapes=[pltpu.VMEM((width, width), BF16), pltpu.VMEM((rows, width), F32)],
        compiler_params=pltpu.CompilerParams(vmem_limit_bytes=24 * 1024 * 1024),
        cost_estimate=pl.CostEstimate(
            flops=2 * 1024 * 1024 * 1024, bytes_accessed=rows * width * 4, transcendentals=0
        ),
        name="make_pool",
    )(pool_in, rim, pool_mix, pool_scale)


def block_place(part, i):
    z, x, _, c = coords()
    j = lax.rem(i, 4)
    s = lax.rem(i, 2)
    if part == 0:
        step = jnp.where(j == 2, 3, jnp.where(j == 3, 1, 0))
    else:
        step = jnp.where(j == 0, 1, jnp.where(j == 1, 3, 2))
    core = jnp.where(i < 4, c, 1 - c)
    side = lax.rem(x + lax.div(x, 2) + s + core, 2)
    return lax.rem(z + step, 4) * 4 + 2 * side + core


def query_place(qi):
    z, x, _, c = coords()
    middle = jnp.logical_or(z == 1, z == 2)
    spot = jnp.where(middle, 4, 0) + 2 * c + jnp.where(z >= 2, 1, 0)
    return jnp.where(lax.rem(x + qi, 2) == 0, spot, 15 - spot)


def scores(q, k):
    return lax.dot_general(q, k, (((1,), (1,)), ((), ())), preferred_element_type=F32)


def diagonal_mask(s):
    row = lax.broadcasted_iota(jnp.int32, (BLK, BLK), 0) // SEGMENT
    col = lax.broadcasted_iota(jnp.int32, (BLK, BLK), 1) // SEGMENT
    return jnp.where(col <= row, s, neg_big)


def with_ones(v):
    return jnp.concatenate([v, jnp.ones((BLK, 128), BF16)], axis=1)


def low_lanes():
    return lax.broadcasted_iota(jnp.int32, (BLK, 128), 1) < HEAD


def split_maps(q):
    zeros = jnp.zeros((BLK, 128), BF16)
    low = low_lanes()
    return jnp.where(low, q, zeros), jnp.where(low, zeros, q)


def sweep(part, kvs, shifted, acc):
    def pair(slot, qi):
        place = block_place(part, slot)
        b_q = query_place(qi)

        def add(masked):
            k = kvs[slot, :, :128]
            v = with_ones(kvs[slot, :, 128:])
            ones = jnp.ones((BLK, 128), BF16)
            low = low_lanes()
            k_ones = (jnp.where(low, k, ones), jnp.where(low, ones, k))
            both = [scores(shifted[2 * qi + m], k_ones[m]) for m in range(2)]
            if masked:
                both = [diagonal_mask(s) for s in both]
            both = [jnp.exp2(s).astype(BF16) for s in both]
            for m in range(2):
                acc[2 * qi + m] += dot(both[m], v)

        pl.when(place < b_q)(functools.partial(add, False))
        pl.when(place == b_q)(functools.partial(add, True))

    def step(t, carry):
        slot, qi = lax.div(t, 2), lax.rem(t, 2)
        pair(slot, qi)
        return carry

    lax.fori_loop(0, 2 * HALF, step, 0)


def attend_a_kernel(q0_ref, q1_ref, *refs):
    kv_refs = refs[:HALF]
    acc, shifted = refs[HALF : HALF + 2]
    (kvs,) = refs[HALF + 2 :]
    for i, ref in enumerate(kv_refs):
        kvs[i] = ref[...]
    acc[...] = jnp.zeros_like(acc)
    k = kv_refs[0][:SAMPLE, :128]
    lane = lax.broadcasted_iota(jnp.int32, (BLK, 128), 1)
    for qi, q_ref in enumerate((q0_ref, q1_ref)):
        for m, q in enumerate(split_maps(q_ref[:BLK])):
            peak = jnp.max(scores(q, k), axis=1, keepdims=True).astype(BF16)
            shifted[2 * qi + m] = jnp.where(lane == (HEAD if m == 0 else 0), -peak, q)
    sweep(0, kvs, shifted, acc)


def attend_a(q0, q1, kvs):
    return pl.pallas_call(
        attend_a_kernel,
        out_shape=(
            jax.ShapeDtypeStruct((4, BLK, 256), F32),
            jax.ShapeDtypeStruct((4, BLK, 128), BF16),
        ),
        in_specs=[VMEM_SPEC, VMEM_SPEC] + [VMEM_SPEC] * HALF,
        out_specs=(VMEM_SPEC, VMEM_SPEC),
        scratch_shapes=[
            pltpu.VMEM((HALF, BLK, 256), BF16),
        ],
        compiler_params=pltpu.CompilerParams(vmem_limit_bytes=32 * 1024 * 1024),
        cost_estimate=pl.CostEstimate(
            flops=9 * 2 * 2 * BLK * BLK * 384, bytes_accessed=HALF * BLK * 512, transcendentals=0
        ),
        name="attend_a",
    )(q0, q1, *kvs)


def attend_b_kernel(gain_ref, q0_ref, q1_ref, before, shifted, *refs):
    kv_refs = refs[:HALF]
    all_refs = refs[HALF:NB] + refs[:HALF]
    out_refs = refs[NB : NB + 2]
    kvs, every, acc, top, kept = refs[NB + 2 :]
    for i, ref in enumerate(kv_refs):
        kvs[i] = ref[...]
    acc[...] = before[...]
    sweep(1, kvs, shifted, acc)
    sums = acc[:, :, 128:]
    fine = jnp.logical_and(jnp.max(sums) < 2.0**100, jnp.min(sums) > 2.0**-60)

    @pl.when(jnp.logical_not(fine))
    def _():
        acc[...] = jnp.zeros_like(acc)
        top[...] = jnp.full_like(top, neg_big)
        for i, ref in enumerate(all_refs):
            every[i] = ref[...]

        def careful(n, carry):
            block, t = lax.div(n, 4), lax.rem(n, 4)
            slot = lax.rem(block, HALF)
            place = jnp.where(block < HALF, block_place(0, slot), block_place(1, slot))
            qi = lax.div(t, 2)
            b_q = query_place(qi)
            low = low_lanes()
            q = jnp.where(qi == 0, q0_ref[:BLK], q1_ref[:BLK])
            zeros = jnp.zeros_like(q)
            q = jnp.where(lax.rem(t, 2) == 0, jnp.where(low, q, zeros), jnp.where(low, zeros, q))

            @pl.when(place <= b_q)
            def _():
                s = scores(q, every[block, :, :128])
                s = jnp.where(place == b_q, diagonal_mask(s), s)
                old = top[t]
                new = jnp.maximum(old, jnp.max(s, axis=1, keepdims=True))
                p = jnp.exp2(s - new[:, :1])
                shrink = jnp.exp2(old - new)
                acc[t] = acc[t] * jnp.concatenate([shrink, shrink], axis=1) + dot(
                    p.astype(BF16), with_ones(every[block, :, 128:])
                )
                top[t] = new

            return carry

        lax.fori_loop(0, 4 * NB, careful, 0)

    _, x, _, _ = coords()
    high = lax.div(x, 2)
    for qi, q_ref in enumerate((q0_ref, q1_ref)):
        lam_parts = q_ref[BLK : BLK + 16].astype(F32)
        lam = (lam_parts[0:1] + lam_parts[1:2]) + lam_parts[2:3]
        one, two = 2 * qi, 2 * qi + 1
        blend = acc[one, :, :128] / acc[one, :, 128:] - lam * (acc[two, :, :128] / acc[two, :, 128:])
        kept[...] = (
            blend
            * lax.rsqrt(jnp.mean(blend * blend, axis=-1, keepdims=True) + eps_norm)
            * gain_ref[...]
            * out_scale
        )
        for t in range(2):
            side = high if t == 0 else 1 - high
            for n in range(4):
                rows = pl.ds(pl.multiple_of((2 * n + side) * 64, 64), 64)
                out_refs[qi][t * 256 + n * 64 : t * 256 + (n + 1) * 64, :] = kept[rows, :].astype(BF16)


def attend_b(gain, q0, q1, before, shifted, kvs, early_kvs):
    out = jax.ShapeDtypeStruct((BLK, VDIM), BF16)
    return pl.pallas_call(
        attend_b_kernel,
        out_shape=(out,) * 2,
        in_specs=[VMEM_SPEC] * 5 + [VMEM_SPEC] * NB,
        out_specs=(VMEM_SPEC,) * 2,
        scratch_shapes=[
            pltpu.VMEM((HALF, BLK, 256), BF16),
            pltpu.VMEM((NB, BLK, 256), BF16),
            pltpu.VMEM((4, BLK, 256), F32),
            pltpu.VMEM((4, BLK, 128), F32),
            pltpu.VMEM((BLK, 128), F32),
        ],
        compiler_params=pltpu.CompilerParams(vmem_limit_bytes=32 * 1024 * 1024),
        cost_estimate=pl.CostEstimate(
            flops=9 * 2 * 2 * BLK * BLK * 384, bytes_accessed=HALF * BLK * 512, transcendentals=0
        ),
        name="attend_b",
    )(gain, q0, q1, before, shifted, *kvs, *early_kvs)


COLS = 1024


def pool_proj_kernel(pm, po, wp, wpo, out_ref):
    out_ref[...] = dot(pm[...], wp[...]) + dot(po[...], wpo[...])


def project_pool(pools, weights):
    out_cols = weights[0].shape[1]
    act = pl.BlockSpec((256, 256), lambda i: (0, 0))
    weight = pl.BlockSpec((256, COLS), lambda i: (0, i))
    return pl.pallas_call(
        pool_proj_kernel,
        grid=(out_cols // COLS,),
        out_shape=jax.ShapeDtypeStruct((256, out_cols), F32),
        in_specs=[act, act, weight, weight],
        out_specs=pl.BlockSpec((256, COLS), lambda i: (0, i)),
        compiler_params=pltpu.CompilerParams(vmem_limit_bytes=24 * 1024 * 1024),
        cost_estimate=pl.CostEstimate(
            flops=2 * 256 * 512 * out_cols, bytes_accessed=8 * 1024 * 1024, transcendentals=0
        ),
        name="project_pool",
    )(*pools, *weights)


def acts_of(refs, blocks):
    z, _, y, _ = coords()
    rows = [pl.ds(pl.multiple_of(lax.rem(y + k, 4) * 64, 64), 64) for k in blocks]
    early = z < 2
    joined = []
    for a, b in (refs[0:2], refs[2:4]):
        one = jnp.concatenate([a[r, :] for r in rows], 0) if len(rows) > 1 else a[rows[0], :]
        two = jnp.concatenate([b[r, :] for r in rows], 0) if len(rows) > 1 else b[rows[0], :]
        joined.append(
            jnp.concatenate([jnp.where(early, one, two), jnp.where(early, two, one)], 1)
        )
    return rows, joined


def halves(i, left, right, value):
    @pl.when(i < 2)
    def _():
        left[...] = value.astype(left.dtype)

    @pl.when(i >= 2)
    def _():
        right[...] = value.astype(right.dtype)


def far_kernel(base, a0, a1, b0, b1, wa, wao, far0, far1):
    rows, (mine, theirs) = acts_of((a0, a1, b0, b1), (2,))
    total = base[rows[0], :] + dot(mine, wa[...]) + dot(theirs, wao[...])
    halves(pl.program_id(0), far0, far1, total)


def rest_kernel(base, a0, a1, b0, b1, wa, wao, own, next0, next1, prev0, prev1):
    i = pl.program_id(0)
    rows, (mine, theirs) = acts_of((a0, a1, b0, b1), (0, 1, 3))
    total = dot(mine, wa[...]) + dot(theirs, wao[...])
    own[...] = total[:64] + base[rows[0], :]
    halves(i, next0, next1, total[64:128] + base[rows[1], :])
    halves(i, prev0, prev1, total[128:] + base[rows[2], :])


def project_out(far, base, backs, swapped, weights):
    out_cols = weights[0].shape[1]
    steps = out_cols // COLS
    mine = pl.BlockSpec((256, 128), lambda i: (0, 0))
    theirs = pl.BlockSpec((256, 128), lambda i: (1, 0))
    weight = pl.BlockSpec((256, COLS), lambda i: (0, i))
    left = pl.BlockSpec((64, COLS), lambda i: (0, jnp.minimum(i, 1)))
    right = pl.BlockSpec((64, COLS), lambda i: (0, jnp.maximum(i - 2, 0)))
    piece = jax.ShapeDtypeStruct((64, out_cols // 2), BF16)
    if far:
        out_shape, out_specs = (piece, piece), (left, right)
    else:
        out_shape = (jax.ShapeDtypeStruct((64, out_cols), F32),) + (piece,) * 4
        out_specs = (pl.BlockSpec((64, COLS), lambda i: (0, i)), left, right, left, right)
    return pl.pallas_call(
        far_kernel if far else rest_kernel,
        grid=(steps,),
        out_shape=out_shape,
        in_specs=[weight, mine, mine, theirs, theirs, weight, weight],
        out_specs=out_specs,
        compiler_params=pltpu.CompilerParams(vmem_limit_bytes=24 * 1024 * 1024),
        cost_estimate=pl.CostEstimate(
            flops=2 * 128 * 512 * out_cols, bytes_accessed=8 * 1024 * 1024, transcendentals=0
        ),
        name="project_far" if far else "project_rest",
    )(base, *backs, *swapped, *weights)


def body(
    tokens,
    norm_gain,
    w_pool_in,
    w_query,
    w_key,
    w_value,
    pool_mix,
    pool_scale,
    lam,
    head_gain,
    pool_proj,
    attn_proj,
):
    _, width = tokens.shape
    gain = norm_gain.reshape(STEPS, 1, width // STEPS)

    kv0, kv1, q0, q1, pool_in, rim = make_front(
        lam, gain, tokens, w_key, w_value, w_query, w_pool_in
    )
    g0, g1 = moved(kv0, kv_pairs(0)), moved(kv1, kv_pairs(1))
    got_q = [moved(q0, q_pairs(0)), moved(q1, q_pairs(1))]
    rim = lax.ppermute(rim, "sp", [(i, i + 1) for i in range(15)])
    up0, down1 = moved(g0, UP), moved(g1, DOWN)
    down0, up1 = moved(g0, DOWN), moved(g1, UP)
    far0, far1 = moved(up0, UP), moved(down1, DOWN)

    def both_cores(arrays):
        return arrays + [moved(a, SWAP) for a in arrays]

    early_kvs = both_cores([g0, g1, up0, down1])
    late_kvs = both_cores([down0, up1, far0, far1])

    pool_mine, pool_theirs = make_pool(pool_in, rim, pool_mix, pool_scale.reshape(1, -1))
    pool_other = moved(pool_theirs, SWAP)
    pool_proj_other = moved(pool_proj, SWAP)
    attn_proj_other = moved(attn_proj, SWAP)

    before, shifted = attend_a(*got_q, early_kvs)
    outs = attend_b(
        head_gain.reshape(1, VDIM), *got_q, before, shifted, late_kvs, early_kvs
    )
    backs = [moved(outs[s], back_pairs(s)) for s in range(2)]
    swapped = [moved(backs[s], SWAP) for s in range(2)]
    base = project_pool((pool_mine, pool_other), (pool_proj, pool_proj_other))
    weights = (attn_proj, attn_proj_other)
    far0, far1 = project_out(True, base, backs, swapped, weights)
    over0, over1 = moved(far0, Y_UP), moved(far1, Y_DOWN)
    mine, next0, next1, prev0, prev1 = project_out(False, base, backs, swapped, weights)
    alone1, alone0 = moved(next1, Y_UP), moved(prev0, Y_DOWN)
    joined0 = moved((next0.astype(F32) + over0.astype(F32)).astype(BF16), Y_UP)
    joined1 = moved((prev1.astype(F32) + over1.astype(F32)).astype(BF16), Y_DOWN)
    half = mine.shape[1] // 2
    left = mine[:, :half] + alone0.astype(F32) + joined0.astype(F32)
    right = mine[:, half:] + alone1.astype(F32) + joined1.astype(F32)
    return jnp.concatenate([left.astype(BF16), right.astype(BF16)], 1)


def solution(mesh):
    return jax.shard_map(
        body,
        mesh=mesh,
        in_specs=(
            P("sp", None),
            P(),
            P(None, "tp"),
            P(None, "tp"),
            P(None, "tp"),
            P(None, "tp"),
            P("tp", None, None),
            P("tp"),
            P("tp"),
            P(),
            P("tp", None),
            P("tp", None),
        ),
        out_specs=P(("sp", "tp"), None),
        check_vma=False,
    )
```
